32 devices in a mesh: sp: 8 (over z, x), tp: 4 (over y, core).
Axes of the slice: x: 2, y: 2, z: 4, core: 2. Of those that a mesh axis runs over, the one named last changes fastest.
Arguments:
- grid_in: bfloat16 [1024, 2048], P('sp', 'tp'), may hold values from -6 to 6
- documents: int32 [1024], P('sp'), may hold values from 0 to 3, never falling along the last dimension, each value on 1 to 512 neighbouring positions
- pre_gain: float32 [2, 2048], replicated, may hold values from 0.1 to 1.9
- query_weight: bfloat16 [2, 2048, 2048], P(None, None, 'tp'), may hold values from -1 to 1
- key_weight: bfloat16 [2, 2048, 2048], P(None, None, 'tp'), may hold values from -4 to 4
- value_weight: bfloat16 [2, 2048, 2048], P(None, None, 'tp'), may hold values from -0.125 to 0.125
- offset_bias: float32 [2, 32, 15, 31], P(None, 'tp'), may hold values from -5 to 5
- out_weight: bfloat16 [2, 2048, 2048], P(None, None, 'tp'), may hold values from -3 to 3
- post_gain: float32 [2, 2048], P(None, 'tp'), may hold values from 0.1 to 1.9
Outputs:
- grid_out: bfloat16 [1024, 2048], P('sp', 'tp')
The draws below stay inside these ranges and needn't reach their ends.
Inputs may be any that keep to these rules, and one draw needn't show every extreme that they name: `documents`: each position's document number; numbers never fall along the token order, and each document covers 1 to 512 positions.
All inputs are finite; a program needn't handle non-finite values.
Results may differ from the reference program's by a relative error of at most 0.0095.
Values may be sent and summed in bfloat16 or wider, within the bound.
A program may use at most 64 MiB of HBM per device.

```python
import math
import jax
import jax.numpy as jnp
import numpy as np
from jax import lax

D = 2048
HEADS = 32
HEAD_DIM = 64
WIN_ROWS = 8
WIN_COLS = 16
GRID_W = 32
LAYERS = 2
TOKENS = 1024
DOCS = 4
DOC_MOST = 512


def paired_weights(key):
    sigma = D ** (-0.5)
    base_draw = jax.random.normal(jax.random.fold_in(key, 101), (LAYERS, D, D), jnp.float32) * sigma
    other_draw = jax.random.normal(jax.random.fold_in(key, 102), (LAYERS, D, D), jnp.float32) * sigma
    return (jnp.clip(base_draw, -6.0 * sigma, 6.0 * sigma), jnp.clip(other_draw, -6.0 * sigma, 6.0 * sigma))


def draw_query_weight(key, part):
    base_draw, other_draw = paired_weights(key)
    return base_draw.astype(jnp.bfloat16)


def draw_key_weight(key, part):
    base_draw, other_draw = paired_weights(key)
    result = other_draw
    return result.astype(jnp.bfloat16)


def draw_out_weight(key, part):
    sigma = D ** (-0.5)
    drawn = jnp.clip(jax.random.normal(jax.random.fold_in(key, 104), (LAYERS, D, D), jnp.float32), -6.0, 6.0) * sigma
    rising = 10.0 ** (jnp.arange(D, dtype=jnp.float32) / D)
    rough = jnp.exp(jax.random.uniform(jax.random.fold_in(key, 105), (LAYERS, 1, D), jnp.float32, -0.4, 0.4))
    return jnp.clip(drawn * rising[None, None, :] * rough, -3.0, 3.0).astype(jnp.bfloat16)


def level_of(own_key, dims, split, smallest, high):
    def one(position, shards_of):
        heights = jax.random.uniform(jax.random.fold_in(jax.random.fold_in(own_key, 6), position), (shards_of,), jnp.float32, smallest / len(split), high / len(split))
        return jnp.repeat(jnp.exp(heights), dims[position] // shards_of).reshape((-1,) + (1,) * (len(dims) - position - 1))

    level = one(*split[0])
    for cut in split[1:]:
        level = level * one(*cut)
    return level


def length_profile(count, total, reach, lean):
    loads = [(1 << 20) // math.isqrt(rank ** lean) + 1 for rank in range(2, count + 1)]
    rest, counts = total - reach - (count - 1), [1] * (count - 1)
    while rest > 0:
        candidates = [i for i in range(count - 1) if counts[i] < reach]
        whole, budget = sum([loads[i] for i in candidates]), rest
        for i in candidates:
            extra = min(reach - counts[i], max(1, budget * loads[i] // whole), rest)
            counts[i] = counts[i] + extra
            rest = rest - extra
    return np.array([reach] + counts)


def uneven_parts(rng, count, total, bound, slope):
    if count == 2:
        one = jax.random.randint(rng, (), max(1, total - bound), min(bound, total - 1) + 1)
        return jnp.stack([one, total - one])
    lengths = jnp.asarray(length_profile(count, total, bound, slope), jnp.int32)
    pairs = (count - 1) // 2
    source_of, taker = lengths[1:1 + 2 * pairs:2], lengths[2:2 + 2 * pairs:2]
    slack = jnp.minimum(source_of - 1, bound - taker)
    passed = jax.random.randint(jax.random.fold_in(rng, 1), (pairs,), 0, 1 << 20) % (slack + 1)
    lengths = lengths.at[1:1 + 2 * pairs:2].set(source_of - passed).at[2:2 + 2 * pairs:2].set(taker + passed)
    return lengths[jax.random.permutation(jax.random.fold_in(rng, 2), count)]


def noise(own_key, dims, spread, reach, shards=(), kind=jnp.bfloat16):
    factor_of = level_of(own_key, dims, shards, -0.22, 0.18) if shards else 1.0
    values = jax.random.normal(own_key, dims, jnp.float32) * spread * factor_of
    return jnp.minimum(jnp.maximum(values, -reach), reach).astype(kind)


def setup_inputs(seed: int = 0) -> dict:
    arg_keys = jax.random.split(jax.random.key(seed), 10)
    grid_in = noise(arg_keys[0], (TOKENS, D), 1.0, 6.0, ((0, 8), (1, 4)))
    documents = jnp.searchsorted(jnp.cumsum(uneven_parts(arg_keys[1], DOCS, TOKENS, DOC_MOST, 0)), jnp.arange(TOKENS), side="right").astype(jnp.int32)
    pre_gain = jnp.clip(1.0 + 0.18 * jax.random.normal(arg_keys[2], (LAYERS, D), jnp.float32), 0.1, 1.9)
    query_weight = draw_query_weight(jax.random.fold_in(arg_keys[9], 71), 0)
    key_weight = draw_key_weight(jax.random.fold_in(arg_keys[9], 71), 0)
    value_weight = noise(arg_keys[5], (LAYERS, D, D), D ** -0.5, 0.125, ((2, 4),))
    offset_bias = noise(arg_keys[6], (LAYERS, HEADS, 2 * WIN_ROWS - 1, 2 * WIN_COLS - 1), 1.0, 5.0, ((1, 4),), jnp.float32)
    out_weight = draw_out_weight(jax.random.fold_in(arg_keys[9], 71), 0)
    post_gain = jnp.clip(1.0 + 0.18 * jax.random.normal(arg_keys[8], (LAYERS, D), jnp.float32), 0.1, 1.9)
    return {"grid_in": grid_in, "documents": documents, "pre_gain": pre_gain, "query_weight": query_weight, "key_weight": key_weight, "value_weight": value_weight, "offset_bias": offset_bias, "out_weight": out_weight, "post_gain": post_gain}


epsilon = 1e-06

def reference(grid_in, documents, pre_gain, query_weight, key_weight, value_weight, offset_bias, out_weight, post_gain):
    tokens_all, model_width = grid_in.shape
    grid_rows = tokens_all // GRID_W
    rim_rows = WIN_ROWS // 2
    score_scale = HEAD_DIM ** (-0.5)
    columns = jnp.arange(GRID_W, dtype=jnp.int32)
    col_start = jnp.clip(columns - WIN_COLS // 2, 0, GRID_W - WIN_COLS)
    col_allowed = (columns[None, :] >= col_start[:, None]) & (columns[None, :] < col_start[:, None] + WIN_COLS)
    col_offset = jnp.clip(columns[None, :] - columns[:, None] + WIN_COLS - 1, 0, 2 * WIN_COLS - 2)
    doc_grid = documents.reshape(grid_rows, GRID_W)
    stream = grid_in
    for layer_index in range(LAYERS):
        widened = stream.astype(jnp.float32)
        scaler = lax.rsqrt(lax.optimization_barrier(jnp.mean(widened * widened, axis=1, keepdims=True)) + epsilon)
        scaled = (widened * pre_gain[layer_index][None, :]).astype(jnp.bfloat16)
        query_rows = (jnp.dot(scaled, query_weight[layer_index], preferred_element_type=jnp.float32) * scaler).astype(jnp.bfloat16)
        key_rows = (jnp.dot(scaled, key_weight[layer_index], preferred_element_type=jnp.float32) * scaler).astype(jnp.bfloat16)
        value_rows = (jnp.dot(scaled, value_weight[layer_index], preferred_element_type=jnp.float32) * scaler).astype(jnp.bfloat16)
        query_grid = query_rows.reshape(grid_rows, GRID_W, HEADS, HEAD_DIM)
        key_grid = key_rows.reshape(grid_rows, GRID_W, HEADS, HEAD_DIM)
        value_grid = value_rows.reshape(grid_rows, GRID_W, HEADS, HEAD_DIM)
        col_bias = offset_bias[layer_index][:, :, col_offset]

        def one_row(row_at):
            slab_start = jnp.clip(row_at - rim_rows, 0, grid_rows - WIN_ROWS).astype(jnp.int32)
            key_slab = lax.dynamic_slice_in_dim(key_grid, slab_start, WIN_ROWS, 0).astype(jnp.float32)
            value_slab = lax.dynamic_slice_in_dim(value_grid, slab_start, WIN_ROWS, 0).astype(jnp.float32)
            doc_slab = lax.dynamic_slice_in_dim(doc_grid, slab_start, WIN_ROWS, 0)
            query_row = lax.dynamic_index_in_dim(query_grid, row_at, 0, keepdims=False).astype(jnp.float32)
            own_docs = lax.dynamic_index_in_dim(doc_grid, row_at, 0, keepdims=False)
            scores = jnp.einsum('chd,jkhd->hcjk', query_row, key_slab) * score_scale
            bias_rows = lax.dynamic_slice_in_dim(col_bias, (slab_start - row_at + WIN_ROWS - 1).astype(jnp.int32), WIN_ROWS, 1)
            scores = scores + jnp.transpose(bias_rows, (0, 2, 1, 3))
            allowed = (doc_slab[None, :, :] == own_docs[:, None, None]) & col_allowed[:, None, :]
            scores = jnp.where(allowed[None], scores, -jnp.inf)
            row_peak = lax.optimization_barrier(jnp.max(scores, axis=(2, 3), keepdims=True))
            lifted = jnp.exp(scores - row_peak)
            weights = (lifted / lax.optimization_barrier(jnp.sum(lifted, axis=(2, 3), keepdims=True))).astype(jnp.bfloat16)
            return jnp.einsum('hcjk,jkhd->chd', weights.astype(jnp.float32), value_slab).astype(jnp.bfloat16)
        attended = lax.map(one_row, jnp.arange(grid_rows, dtype=jnp.int32)).reshape(tokens_all, model_width)
        branch = jnp.dot(attended, out_weight[layer_index], preferred_element_type=jnp.float32)
        branch_scale = lax.rsqrt(lax.optimization_barrier(jnp.mean(branch * branch, axis=1, keepdims=True)) + epsilon)
        stream = (widened + branch * branch_scale * post_gain[layer_index][None, :]).astype(jnp.bfloat16)
    return stream
```

```python
import functools

import jax
import jax.numpy as jnp
from jax import lax
from jax.experimental import pallas as pl
from jax.experimental.pallas import tpu as pltpu
from jax.sharding import PartitionSpec as P

HEAD_DIM = 64
WIN_ROWS = 8
WIN_COLS = 16
GRID_W = 32
LAYERS = 2
EPS = 1e-06
MESH = pl.DeviceIdType.MESH
F32 = jnp.float32
BF16 = jnp.bfloat16


def kernel(
    nsp, ntp, heads, chunks, x_hbm, doc_hbm, pre_hbm, ob_hbm, post_hbm, wq_hbm, wk_hbm, wv_hbm, wo_hbm,
    out_ref,
    xg, bg, att, docs, pg, ssq, w_all, xs, qb, kb, vb, mask, bias, fb, doc_ref, pre_ref, ob_ref,
    w_sem, loc_sem, sp_s, sp_r, y_s, y_r, p_s, p_r, ay_s, ay_r, ap_s, ap_r, d_s, d_r, g_s, g_r, q_s, q_r,
):
    s = lax.axis_index("sp")
    t = lax.axis_index("tp")
    nc = ntp // 2
    n, feat = x_hbm.shape
    width = feat * ntp
    keys = 3 * n
    pairs = heads // 2
    row_count = n // GRID_W
    rim = WIN_ROWS // 2
    core = lax.rem(t, 2)
    partner = t + 1 - 2 * core
    odd = lax.rem(s, 2)
    step = 1 - 2 * odd
    s_near = s + step
    near_row = 2 - 2 * odd
    far_row = 2 * odd
    up = s + 2 * step
    has_up = (up >= 0) & (up < nsp)
    down = s - 2 * step
    has_far = (down >= 0) & (down < nsp)
    s_up = jnp.clip(up, 0, nsp - 1)
    s_down = jnp.clip(down, 0, nsp - 1)
    size = n // chunks
    late = chunks // 2

    def y_to(d):
        return lax.rem(t + 2 * d, ntp)

    def y_from(d):
        return lax.rem(t + ntp - 2 * d, ntp)

    def tp_to(d):
        return lax.rem(t + d, ntp)

    def tp_from(d):
        return lax.rem(t + ntp - d, ntp)

    barrier = pltpu.get_barrier_semaphore()
    for d in range(1, ntp):
        pl.semaphore_signal(barrier, inc=1, device_id=(s, tp_to(d)), device_id_type=MESH)
    pl.semaphore_signal(barrier, inc=1, device_id=(s_near, t), device_id_type=MESH)

    @pl.when(has_up)
    def _():
        pl.semaphore_signal(barrier, inc=1, device_id=(s_up, t), device_id_type=MESH)

    @pl.when(has_far)
    def _():
        pl.semaphore_signal(barrier, inc=1, device_id=(s_down, t), device_id_type=MESH)

    locals_in = []
    for k, (src, dst) in enumerate((
        (x_hbm, xg.at[t, pl.ds(n, n)]), (doc_hbm, doc_ref), (post_hbm, pg.at[t]), (ob_hbm, ob_ref), (pre_hbm, pre_ref),
    )):
        c = pltpu.make_async_copy(src, dst, loc_sem.at[k])
        c.start()
        locals_in.append(c)
    pl.semaphore_wait(barrier, ntp + has_up.astype(jnp.int32) + has_far.astype(jnp.int32))

    def remote(src, dst, ss, rs, dev):
        return pltpu.make_async_remote_copy(
            src_ref=src, dst_ref=dst, send_sem=ss, recv_sem=rs, device_id=dev, device_id_type=MESH
        )

    sends = []

    def run_if(cond, fn):
        if cond is None:
            fn()
        else:
            pl.when(cond)(fn)

    def go(c, cond=None):
        run_if(cond, c.start)
        sends.append((c, cond))

    def fire(c, cond=None):
        run_if(cond, c.start)

    def finish():
        for c, cond in sends:
            run_if(cond, c.wait_send)
        sends.clear()

    def drain(ref, sem, cond=None):
        run_if(cond, remote(ref, ref, sem, d_r.at[0], (s, partner)).wait_send)

    def drain_gather(g, buf):
        part = n - late * size
        for k in range(3):
            cond = has_far if k == far else None
            drain(buf.at[pl.ds(0, nc), pl.ds(0, n)], p_s.at[g, k], cond)
            drain(buf.at[pl.ds(0, nc - 1), pl.ds(0, n if k == own else late * size)], y_s.at[g, k], cond)
        for k, cond in ((0, None), (1, has_up)):
            drain(buf.at[0, pl.ds(0, n)], sp_s.at[g, k, 0], cond)
            drain(buf.at[pl.ds(0, nc - 1), pl.ds(0, part)], sp_s.at[g, k, 1], cond)

    def drain_att(l):
        drain(att.at[l, pl.ds(0, nc - 1)], ay_s.at[l])
        drain(att.at[l, pl.ds(0, nc)], ap_s.at[l])

    own, near, far = 0, 1, 2
    base_of = {own: n, near: near_row * n, far: far_row * n}
    u_base = (2 - near_row) * n

    def at(base, c):
        return pl.ds(pl.multiple_of(base + c * size, size), size)

    def p_send(g, buf, k, d, c, cond=None):
        blk = buf.at[y_from(d) if d else t, at(base_of[k], c)]
        fire(remote(blk, blk, p_s.at[g, k], p_r.at[g, k], (s, partner)), cond)

    def y_send(g, buf, k, c, cond=None):
        blk = buf.at[t, at(base_of[k], c)]
        for d in range(1, nc):
            fire(remote(blk, blk, y_s.at[g, k], y_r.at[g, k, d - 1, c], (s, y_to(d))), cond)

    def y_recv(g, buf, k, d, c, cond=None):
        blk = buf.at[y_from(d), at(base_of[k], c)]
        run_if(cond, remote(blk, blk, y_s.at[g, k], y_r.at[g, k, d - 1, c], (s, partner)).wait_recv)
        p_send(g, buf, k, d, c, cond)

    def near_send(g, buf, d, c):
        who = y_from(d) if d else t
        fire(
            remote(
                buf.at[who, at(n, c)], buf.at[who, at(u_base, c)],
                sp_s.at[g, 0, min(d, 1)], sp_r.at[g, 0, d, c], (s_near, t),
            )
        )

    def near_recv(g, buf, d, c):
        who = y_from(d) if d else t
        blk = buf.at[who, at(base_of[near], c)]
        remote(blk, blk, sp_s.at[g, 0, 0], sp_r.at[g, 0, d, c], (s, partner)).wait_recv()
        fire(
            remote(
                blk, buf.at[who, at(base_of[far], c)],
                sp_s.at[g, 1, min(d, 1)], sp_r.at[g, 1, d, c], (s_up, t),
            ),
            has_up,
        )
        if c < late:
            y_send(g, buf, near, c)
        p_send(g, buf, near, d, c)

    def far_recv(g, buf, d, c):
        who = y_from(d) if d else t
        blk = buf.at[who, at(base_of[far], c)]
        run_if(has_far, remote(blk, blk, sp_s.at[g, 1, 0], sp_r.at[g, 1, d, c], (s, partner)).wait_recv)
        if c < late:
            y_send(g, buf, far, c, has_far)
        p_send(g, buf, far, d, c, has_far)

    def own_recv(g, buf, d, c):
        y_recv(g, buf, own, d, c)
        if c >= late:
            near_send(g, buf, d, c)

    def start_own(g, buf):
        for c in list(range(late, chunks)) + list(range(late)):
            y_send(g, buf, own, c)
        for c in range(chunks):
            near_send(g, buf, 0, c)
        for c in range(chunks):
            p_send(g, buf, own, 0, c)

    def relay(g, buf):
        others = range(1, nc)
        for i in range(late):
            near_recv(g, buf, 0, i)
            for d in others:
                own_recv(g, buf, d, late + i)
        for i in range(late):
            near_recv(g, buf, 0, late + i)
            for d in others:
                own_recv(g, buf, d, i)
        for i in range(late):
            far_recv(g, buf, 0, i)
            for d in others:
                near_recv(g, buf, d, late + i)
                y_recv(g, buf, near, d, i)

    def relay_far(g, buf):
        others = range(1, nc)
        for i in range(late):
            far_recv(g, buf, 0, late + i)
        for i in range(late):
            for d in others:
                y_recv(g, buf, far, d, i, has_far)
                far_recv(g, buf, d, late + i)

    def wait_p(g, k, buf, cond=None):
        blk = buf.at[pl.ds(0, nc), pl.ds(0, n)]
        run_if(cond, remote(blk, blk, p_s.at[g, k], p_r.at[g, k], (s, partner)).wait_recv)

    locals_in[0].wait()
    locals_in[1].wait()
    locals_in[2].wait()
    doc_near = remote(doc_ref, docs.at[0], d_s.at[0], d_r.at[0], (s_near, t))
    doc_far = remote(docs.at[0], docs.at[1], d_s.at[1], d_r.at[1], (s_up, t))
    go(doc_near)
    start_own(0, xg)
    w_copies = []
    for l in range(LAYERS):
        for j, w in enumerate((wq_hbm, wk_hbm, wv_hbm, wo_hbm)):
            c = pltpu.make_async_copy(w.at[l], w_all.at[l, j], w_sem.at[l, j])
            c.start()
            w_copies.append(c)
    for d in range(1, ntp):
        go(remote(pg.at[t], pg.at[t], g_s.at[d], g_r.at[d], (s, tp_to(d))))
    for c in locals_in[3:]:
        c.wait()

    span = fb.shape[2]
    for l in range(LAYERS):
        fb[l] = jnp.zeros_like(fb[l])
        for dr in range(2 * WIN_ROWS - 1):
            fb[l, :, dr * GRID_W:dr * GRID_W + 2 * WIN_COLS - 1] = ob_ref[l, dr]
    shift = span - ((WIN_ROWS - 1 - rim) * GRID_W + WIN_COLS - 1)

    def make_bias(i, _):
        line = jnp.broadcast_to(fb[i // heads, pl.ds(i % heads, 1), :], (n, span))
        bias[i] = pltpu.roll(line, shift, 1, stride=1, stride_axis=0)[:, :keys]
        return 0

    lax.fori_loop(0, heads, make_bias, 0)
    doc_near.wait_recv()
    go(doc_far, has_up)

    @pl.when(jnp.logical_not(has_far))
    def _():
        docs[1] = jnp.zeros_like(docs[1])
        rr = pl.ds(pl.multiple_of(far_row * n, n), n)
        kb[rr, :] = jnp.zeros((n, feat), BF16)
        vb[rr, :] = jnp.zeros((n, feat), BF16)

    own_docs = doc_ref[...].astype(F32)
    q_docs = jnp.transpose(jnp.broadcast_to(own_docs, (n, n)))
    qi = lax.broadcasted_iota(jnp.int32, (n, n), 0)
    ki = lax.broadcasted_iota(jnp.int32, (n, n), 1)
    all_rows = row_count * nsp
    q_row = s * row_count + qi // GRID_W
    q_col = qi % GRID_W
    a = jnp.clip(q_row - rim, 0, all_rows - WIN_ROWS)
    cs = jnp.clip(q_col - WIN_COLS // 2, 0, GRID_W - WIN_COLS)
    k_col = ki % GRID_W
    col_ok = (k_col >= cs) & (k_col < cs + WIN_COLS)
    relay(0, xg)
    run_if(has_far, doc_far.wait_recv)
    near_docs = docs[0].astype(F32)
    far_docs = docs[1].astype(F32)
    odd_f = odd.astype(F32)
    prev_docs = near_docs * odd_f + far_docs * (1.0 - odd_f)
    next_docs = far_docs * odd_f + near_docs * (1.0 - odd_f)
    for b, k_docs in enumerate((prev_docs, own_docs, next_docs)):
        k_row = (s + b - 1) * row_count + ki // GRID_W
        ok = (k_row >= a) & (k_row < a + WIN_ROWS) & col_ok
        ok = ok & (q_docs == jnp.broadcast_to(k_docs, (n, n)))
        mask[:, b * n:(b + 1) * n] = jnp.where(ok, 0.0, -jnp.inf)

    def qkv(l, k):
        r = pl.ds(pl.multiple_of(base_of[k], n), n)
        if l == 1:
            total = jnp.zeros((n, 1), F32)
            for j in range(ntp):
                br = bg[j, r, :].astype(F32)
                total = total + jnp.sum(br * br, axis=1, keepdims=True)
            scale = lax.rsqrt(total / width + EPS)
        stat = jnp.zeros((n, 1), F32)
        for j in range(ntp):
            xv = xg[j, r, :].astype(F32)
            if l == 1:
                br = bg[j, r, :].astype(F32)
                xn = (xv + br * scale * pg[j, 0:1, :]).astype(BF16)
                if k == own:
                    xg[j, r, :] = xn
                xv = xn.astype(F32)
            stat = stat + jnp.sum(xv * xv, axis=1, keepdims=True)
            xs[:, j * feat:(j + 1) * feat] = (xv * pre_ref[l:l + 1, j * feat:(j + 1) * feat]).astype(BF16)
        scaler = lax.rsqrt(stat / width + EPS)
        if k == own:
            qb[...] = (jnp.dot(xs[...], w_all[l, 0], preferred_element_type=F32) * scaler).astype(BF16)
        kb[r, :] = (jnp.dot(xs[...], w_all[l, 1], preferred_element_type=F32) * scaler).astype(BF16)
        vb[r, :] = (jnp.dot(xs[...], w_all[l, 2], preferred_element_type=F32) * scaler).astype(BF16)

    pw = 2 * HEAD_DIM
    lane = lax.broadcasted_iota(jnp.int32, (n, pw), 1)
    low = lane < HEAD_DIM
    score_scale = HEAD_DIM ** (-0.5)

    def attend(l, group):
        scs = []
        for p in group:
            q2 = qb[:, p * pw:(p + 1) * pw]
            k2 = kb[:, p * pw:(p + 1) * pw]
            for e in range(2):
                qe = jnp.where(low if e == 0 else ~low, q2, jnp.zeros_like(q2))
                sc = lax.dot_general(qe, k2, (((1,), (1,)), ((), ())), preferred_element_type=F32)
                scs.append(sc * score_scale + bias[l * heads + 2 * p + e] + mask[...])
        exs = [jnp.exp(sc - jnp.max(sc, axis=1, keepdims=True)) for sc in scs]
        for i, p in enumerate(group):
            v2 = vb[:, p * pw:(p + 1) * pw]
            outs = []
            for e in range(2):
                ex = exs[2 * i + e]
                o = jnp.dot(ex.astype(BF16), v2, preferred_element_type=F32)
                outs.append(o / jnp.sum(ex, axis=1, keepdims=True))
            att[l, t, p] = jnp.where(low, outs[0], outs[1]).astype(BF16)

    def send_att(l, p):
        blk = att.at[l, t, p]
        for d in range(1, nc):
            fire(remote(blk, blk, ay_s.at[l], ay_r.at[l, d - 1, p], (s, y_to(d))))
        fire(remote(blk, blk, ap_s.at[l], ap_r.at[l, 0], (s, partner)))

    def part_dot(l, who):
        wide = jnp.concatenate([att[l, who, p] for p in range(pairs)], axis=1)
        wrows = pl.ds(pl.multiple_of(who * feat, feat), feat)
        return jnp.dot(wide, w_all[l, 3, wrows, :], preferred_element_type=F32)

    def out_proj(l):
        acc = part_dot(l, t)
        for p in range(pairs):
            for d in range(1, nc):
                blk = att.at[l, y_from(d), p]
                remote(blk, blk, ay_s.at[l], ay_r.at[l, d - 1, p], (s, partner)).wait_recv()
                fire(remote(blk, blk, ap_s.at[l], ap_r.at[l, d], (s, partner)))
        for d in range(nc):
            who = lax.rem(partner + ntp - 2 * d, ntp)
            if d > 0:
                acc = acc + part_dot(l, y_from(d))
            blk = att.at[l, who]
            remote(blk, blk, ap_s.at[l], ap_r.at[l, d], (s, partner)).wait_recv()
            acc = acc + part_dot(l, who)
        return acc

    for l in range(LAYERS):
        buf = xg if l == 0 else bg
        if l == 1:
            relay(1, bg)
        wait_p(l, own, buf)
        for c in w_copies[4 * l:4 * l + 4]:
            c.wait()
        qkv(l, own)
        relay_far(l, buf)
        wait_p(l, near, buf)
        qkv(l, near)
        wait_p(l, far, buf, has_far)
        pl.when(has_far)(lambda l=l: qkv(l, far))
        for first in range(0, pairs, 2):
            group = list(range(first, min(first + 2, pairs)))
            attend(l, group)
            for p in group:
                send_att(l, p)
        branch = out_proj(l)
        if l == 0:
            bg[t, n:2 * n, :] = branch.astype(BF16)
            start_own(1, bg)
            finish()
            drain_gather(0, xg)
            drain_att(0)
            lax.fori_loop(heads, 2 * heads, make_bias, 0)
            for d in range(1, ntp):
                blk = pg.at[tp_from(d)]
                remote(blk, blk, g_s.at[d], g_r.at[d], (s, partner)).wait_recv()

    part = jnp.sum(branch * branch, axis=1, keepdims=True)
    flat = jnp.transpose(jnp.broadcast_to(part, (n, n)))[0:8, :]
    ssq[t] = flat
    for d in range(1, ntp):
        go(remote(ssq.at[t], ssq.at[t], q_s.at[d], q_r.at[d], (s, tp_to(d))))
    for d in range(1, ntp):
        blk = ssq.at[tp_from(d)]
        remote(blk, blk, q_s.at[d], q_r.at[d], (s, partner)).wait_recv()
    total = ssq[0]
    for j in range(1, ntp):
        total = total + ssq[j]
    scale_row = lax.rsqrt(total[0:1, :] / width + EPS)
    scale = jnp.transpose(jnp.broadcast_to(scale_row, (n, n)))[:, 0:1]
    out_ref[...] = (xg[t, n:2 * n, :].astype(F32) + branch * scale * pg[t, 1:2, :]).astype(BF16)
    finish()
    drain_gather(1, bg)
    drain_att(1)


def solution(mesh):
    nsp, ntp = mesh.shape["sp"], mesh.shape["tp"]

    def shards(grid_in, documents, pre_gain, wq, wk, wv, offset_bias, wo, post_gain):
        n, feat = grid_in.shape
        heads = offset_bias.shape[1]
        width = pre_gain.shape[1]
        span = 4 * n
        table = offset_bias.transpose(0, 2, 1, 3)
        chunks = n // GRID_W
        nc, pairs = ntp // 2, heads // 2
        dma = pltpu.SemaphoreType.DMA
        vm = pl.BlockSpec(memory_space=pltpu.VMEM)
        hb = pl.BlockSpec(memory_space=pltpu.HBM)
        return pl.pallas_call(
            functools.partial(kernel, nsp, ntp, heads, chunks),
            out_shape=pltpu.VMEM((n, feat), BF16),
            in_specs=[hb] * 9,
            out_specs=vm,
            scratch_shapes=[
                pltpu.VMEM((ntp, 3 * n, feat), BF16),
                pltpu.VMEM((ntp, 3 * n, feat), BF16),
                pltpu.VMEM((LAYERS, ntp, pairs, n, 2 * HEAD_DIM), BF16),
                pltpu.VMEM((2, 1, n), jnp.int32),
                pltpu.VMEM((ntp, LAYERS, feat), F32),
                pltpu.VMEM((ntp, 8, n), F32),
                pltpu.VMEM((LAYERS, 4, width, feat), BF16),
                pltpu.VMEM((n, width), BF16),
                pltpu.VMEM((n, feat), BF16),
                pltpu.VMEM((3 * n, feat), BF16),
                pltpu.VMEM((3 * n, feat), BF16),
                pltpu.VMEM((n, 3 * n), F32),
                pltpu.VMEM((LAYERS * heads, n, 3 * n), F32),
                pltpu.VMEM((LAYERS, heads, span), F32),
                pltpu.VMEM((1, n), jnp.int32),
                pltpu.VMEM((LAYERS, width), F32),
                pltpu.VMEM(table.shape, F32),
                dma((LAYERS, 4)),
                dma((5,)),
                dma((2, 2, 2)), dma((2, 2, nc, chunks)),
                dma((2, 3)), dma((2, 3, nc - 1, chunks)),
                dma((2, 3)), dma((2, 3)),
                dma((2,)), dma((2, nc - 1, pairs)),
                dma((2,)), dma((2, nc)),
                dma((2,)), dma((2,)),
                dma((ntp,)), dma((ntp,)),
                dma((ntp,)), dma((ntp,)),
            ],
            compiler_params=pltpu.CompilerParams(
                collective_id=0, has_side_effects=True, vmem_limit_bytes=58 * 1024 * 1024
            ),
        )(grid_in, documents.reshape(1, n), pre_gain, table, post_gain, wq, wk, wv, wo)

    return jax.shard_map(
        shards,
        mesh=mesh,
        in_specs=(
            P("sp", "tp"),
            P("sp"),
            P(),
            P(None, None, "tp"),
            P(None, None, "tp"),
            P(None, None, "tp"),
            P(None, "tp", None, None),
            P(None, None, "tp"),
            P(None, "tp"),
        ),
        out_specs=P("sp", "tp"),
        check_vma=False,
    )
```
